32 devices in a mesh: ep: 8 (over z, y), tp: 4 (over x, core).
Axes of the slice: x: 2, y: 2, z: 4, core: 2. Of those that a mesh axis runs over, the one named last changes fastest.
Arguments:
- tokens: bfloat16 [384, 2048], P('ep'), may hold values from -6 to 6
- out_grad: bfloat16 [384, 2048], P('ep'), may hold values from -4 to 4
- expert_ids: int32 [384, 4], P('ep'), may hold values from 0 to 7, all different within a row; in each aligned block of 48 rows (0 to 47, 48 to 95, ...) at most 48 rows name the same one
- router_weight: bfloat16 [2048, 8], replicated, may hold values from -0.125 to 0.125
- w_gate: bfloat16 [8, 2048, 1536], P('ep', None, 'tp'), may hold values from -0.125 to 0.125
- w_up: bfloat16 [8, 2048, 1536], P('ep', None, 'tp'), may hold values from -0.125 to 0.125
- w_down: bfloat16 [8, 1536, 2048], P('ep', 'tp'), may hold values from -0.15625 to 0.15625
Outputs:
- token_grad: bfloat16 [384, 2048], P('ep', 'tp')
- router_grad: float32 [2048, 8], P('tp', 'ep')
- w_gate_grad: bfloat16 [8, 2048, 1536], P('ep', None, 'tp')
- w_up_grad: bfloat16 [8, 2048, 1536], P('ep', None, 'tp')
- w_down_grad: bfloat16 [8, 1536, 2048], P('ep', 'tp')
The draws below stay inside these ranges and needn't reach their ends.
Inputs may be any that keep to these rules, and one draw needn't show every extreme that they name: `expert_ids`: each row names 4 different experts; among the rows of one device no expert is named more than 48 times, and in some devices' rows one expert is named exactly 48 times.
All inputs are finite; a program needn't handle non-finite values.
Results may differ from the reference program's by a relative error of at most 0.0058.
Values may be sent and summed in bfloat16 or wider, within the bound.
A program may use at most 128 MiB of HBM per device.

```python
import math
import jax
import jax.numpy as jnp
import numpy as np
from jax import lax

D = 2048
FF = 1536
TOPK = 4
TOK_DEV = 48
EXPERTS = 8
TOKENS = 384
CAP = 48
N_EP = 8


def draw_tokens(key, part):
    base_key = jax.random.fold_in(key, 11)
    pick_key = jax.random.fold_in(key, 12)
    base = jax.random.normal(base_key, (TOKENS, D), jnp.float32)
    strong = jax.random.randint(pick_key, (TOKENS, 1), 0, 16) == 0
    values = jnp.where(strong, 4.0 * base, base)
    return jnp.clip(values, -6.0, 6.0).astype(jnp.bfloat16)


def shard_levels(stream_key, shape, pieces, least, high):
    def one(dim, parts):
        steps = jax.random.uniform(jax.random.fold_in(jax.random.fold_in(stream_key, 6), dim), (parts,), jnp.float32, least / len(pieces), high / len(pieces))
        return jnp.repeat(jnp.exp(steps), shape[dim] // parts).reshape((-1,) + (1,) * (len(shape) - dim - 1))

    factor_of = one(*pieces[0])
    for cut in pieces[1:]:
        factor_of = factor_of * one(*cut)
    return factor_of


def shared_out(stream_key, own, number, rows, amount, top, bound, skew):
    ranking = jax.random.permutation(stream_key, amount)
    heavy_load, ordinary = shares(amount, rows * top, bound, skew, True), shares(amount, rows * top, bound, skew, False)
    places = jnp.arange(amount)

    def named(sizes, rotation):
        used = int((sizes > 0).sum())
        fixed = max(1, used // 4)
        moved = fixed + (places - fixed + rotation * (used - fixed)) % max(1, amount - fixed)
        return jnp.zeros((amount,), jnp.int32).at[ranking[jnp.where(places < fixed, places, moved)]].set(jnp.asarray(sizes, jnp.int32))

    sizes = jnp.where(number % 4 == 0, named(heavy_load, number // 4), named(ordinary, number - number // 4 - 1))
    mixed = jax.random.permutation(jax.random.fold_in(own, 3), amount)
    donor, taker = mixed[0:amount // 2 * 2:2], mixed[1:amount // 2 * 2:2]
    slack = jnp.minimum(sizes[donor] - 1, bound - sizes[taker]) // 2
    slack = jnp.where((donor == ranking[0]) | (taker == ranking[0]) | (sizes[taker] == 0), 0, jnp.maximum(slack, 0))
    moved = jax.random.randint(jax.random.fold_in(own, 4), (amount // 2,), 0, 1 << 20) % (slack + 1)
    sizes = sizes.at[donor].add(-moved).at[taker].add(moved)
    items = jnp.searchsorted(jnp.cumsum(sizes), jnp.arange(rows * top), side="right").astype(jnp.int32)
    table = items.reshape(top, rows).T
    table = table[jax.random.permutation(jax.random.fold_in(own, 1), rows)]
    rotation = jax.random.randint(jax.random.fold_in(own, 2), (rows, 1), 0, top)
    return jnp.take_along_axis(table, (jnp.arange(top)[None, :] + rotation) % top, axis=1)


def shares(number_of, total, reach, lean, full):
    portions = [(1 << 20) // math.isqrt(standing ** lean) + 1 for standing in range(1, number_of + 1)]
    largest = reach if full else min(reach, max(-(-total // number_of), total * portions[0] // sum(portions)))
    least = 1 if total - largest >= number_of - 1 else 0
    given, surplus = [largest] + [least] * (number_of - 1), total - largest - least * (number_of - 1)
    while surplus > 0:
        free = [i for i in range(1, number_of) if given[i] < largest] or [i for i in range(1, number_of) if given[i] < reach]
        mass, budget = sum([portions[i] for i in free]), surplus
        for i in free:
            more = min(reach - given[i], max(1, budget * portions[i] // mass), surplus)
            given[i] = given[i] + more
            surplus = surplus - more
    return np.array(given)


def gaussian(key, shape, deviation, bound, pieces=(), kind=jnp.bfloat16):
    values = deviation * jax.random.normal(key, shape, jnp.float32)
    if pieces:
        values = values * shard_levels(key, shape, pieces, -0.22, 0.18)
    return jnp.clip(values, -bound, bound).astype(kind)


def setup_inputs(seed: int = 0) -> dict:
    seeds = jax.random.split(jax.random.key(seed), 8)
    tokens = draw_tokens(jax.random.fold_in(seeds[7], 71), 0)
    out_grad = gaussian(seeds[1], (TOKENS, D), 0.3, 4.0, ((0, 8),))
    expert_ids_keys = jax.random.split(jax.random.fold_in(seeds[2], 1), TOKENS // TOK_DEV)
    expert_ids_turns = jax.random.permutation(jax.random.fold_in(seeds[2], 3), TOKENS // TOK_DEV)
    expert_ids = jax.vmap(lambda own, number: shared_out(jax.random.fold_in(seeds[2], 2), own, number, TOK_DEV, EXPERTS, TOPK, CAP, 1))(expert_ids_keys, expert_ids_turns).reshape((TOKENS, TOPK))
    router_weight = gaussian(seeds[3], (D, EXPERTS), D ** -0.5, 0.125)
    w_gate = gaussian(seeds[4], (EXPERTS, D, FF), D ** -0.5, 0.125, ((0, 8), (2, 4)))
    w_up = gaussian(seeds[5], (EXPERTS, D, FF), D ** -0.5, 0.125, ((0, 8), (2, 4)))
    w_down = gaussian(seeds[6], (EXPERTS, FF, D), FF ** -0.5, 0.15625, ((0, 8), (1, 4)))
    return {"tokens": tokens, "out_grad": out_grad, "expert_ids": expert_ids, "router_weight": router_weight, "w_gate": w_gate, "w_up": w_up, "w_down": w_down}


def activation_parts(gate_pre, up_pre):
    glu = jnp.minimum(gate_pre, 7.0)
    linear = jnp.clip(up_pre, -7.0, 7.0)
    sigma = jax.nn.sigmoid(1.702 * glu)
    act_value = glu * sigma
    hidden = (linear + 1.0) * act_value
    slope = (linear + 1.0) * (sigma + 1.702 * glu * sigma * (1.0 - sigma))
    slope = jnp.where(gate_pre < 7.0, slope, 0.0)
    up_slope = jnp.where((up_pre > -7.0) & (up_pre < 7.0), act_value, 0.0)
    return hidden, slope, up_slope


def reference(tokens, out_grad, expert_ids, router_weight, w_gate, w_up, w_down):
    logits = jnp.dot(tokens, router_weight, preferred_element_type=jnp.float32)
    chosen = jnp.take_along_axis(logits, expert_ids, axis=1)
    gate_values = jax.nn.softmax(chosen, axis=-1)
    assign_total = TOKENS * TOPK
    slot_total = N_EP * CAP
    flat_ids = expert_ids.reshape(-1)
    flat_tok = (jnp.arange(assign_total, dtype=jnp.int32) // TOPK).astype(jnp.int32)
    flat_gate = gate_values.reshape(-1)

    def per_expert(carry, inputs):
        token_acc, score_acc = carry
        gate_mat, up_mat, down_mat, expert = inputs
        picked = jnp.nonzero(flat_ids == expert, size=slot_total, fill_value=assign_total)[0].astype(jnp.int32)
        valid = picked < assign_total
        safe_pick = jnp.minimum(picked, assign_total - 1).astype(jnp.int32)
        tok_rows = flat_tok[safe_pick]
        inputs_rows = tokens[tok_rows]
        grad_rows = out_grad[tok_rows]
        weight_rows = jnp.where(valid, flat_gate[safe_pick], 0.0)
        gate_pre = jnp.dot(inputs_rows, gate_mat, preferred_element_type=jnp.float32)
        up_pre = jnp.dot(inputs_rows, up_mat, preferred_element_type=jnp.float32)
        hidden, slope, up_slope = activation_parts(gate_pre, up_pre)
        back_proj = jnp.dot(grad_rows, down_mat.T, preferred_element_type=jnp.float32)
        gate_score = jnp.sum(hidden * back_proj, axis=1)
        d_hidden = weight_rows[:, None] * back_proj
        d_gate_pre = (d_hidden * slope).astype(jnp.bfloat16)
        d_up_pre = (d_hidden * up_slope).astype(jnp.bfloat16)
        weighted = (weight_rows[:, None] * hidden).astype(jnp.bfloat16)
        down_grad = jnp.dot(weighted.T, grad_rows, preferred_element_type=jnp.float32).astype(jnp.bfloat16)
        gate_grad = jnp.dot(inputs_rows.T, d_gate_pre, preferred_element_type=jnp.float32).astype(jnp.bfloat16)
        up_grad = jnp.dot(inputs_rows.T, d_up_pre, preferred_element_type=jnp.float32).astype(jnp.bfloat16)
        token_part = jnp.dot(d_gate_pre, gate_mat.T, preferred_element_type=jnp.float32)
        token_part = token_part + jnp.dot(d_up_pre, up_mat.T, preferred_element_type=jnp.float32)
        token_acc = token_acc.at[tok_rows].add(jnp.where(valid[:, None], token_part, 0.0))
        score_acc = score_acc.at[safe_pick].add(jnp.where(valid, gate_score, 0.0))
        return (token_acc, score_acc), (gate_grad, up_grad, down_grad)

    start_carry = (jnp.zeros((TOKENS, D), jnp.float32), jnp.zeros((assign_total,), jnp.float32))
    expert_list = jnp.arange(EXPERTS, dtype=jnp.int32)
    (token_acc, score_acc), (w_gate_grad, w_up_grad, w_down_grad) = lax.scan(
        per_expert, start_carry, (w_gate, w_up, w_down, expert_list))
    gate_score = score_acc.reshape(TOKENS, TOPK)
    d_chosen = gate_values * (gate_score - jnp.sum(gate_values * gate_score, axis=-1, keepdims=True))
    one_hot = (expert_ids[:, :, None] == jnp.arange(EXPERTS, dtype=jnp.int32)[None, None, :]).astype(jnp.float32)
    d_logits = jnp.sum(d_chosen[:, :, None] * one_hot, axis=1)
    router_grad = jnp.dot(tokens.astype(jnp.float32).T, d_logits, precision=lax.Precision.HIGHEST)
    router_part = jnp.dot(d_logits, router_weight.astype(jnp.float32).T, precision=lax.Precision.HIGHEST)
    token_grad = (token_acc + router_part).astype(jnp.bfloat16)
    return token_grad, router_grad, w_gate_grad, w_up_grad, w_down_grad
```

```python
import functools
import jax
import jax.numpy as jnp
from jax import lax
from jax.experimental import pallas as pl
from jax.experimental.pallas import tpu as pltpu
from jax.sharding import PartitionSpec as P

MESH = pl.DeviceIdType.MESH


def activation_parts(gate_pre, up_pre):
    glu = jnp.minimum(gate_pre, 7.0)
    linear = jnp.clip(up_pre, -7.0, 7.0)
    sigma = jax.nn.sigmoid(1.702 * glu)
    act_value = glu * sigma
    hidden = (linear + 1.0) * act_value
    slope = (linear + 1.0) * (sigma + 1.702 * glu * sigma * (1.0 - sigma))
    slope = jnp.where(gate_pre < 7.0, slope, 0.0)
    up_slope = jnp.where((up_pre > -7.0) & (up_pre < 7.0), act_value, 0.0)
    return (hidden, slope, up_slope)


def contract_last(left, right):
    return lax.dot_general(
        left, right, (((1,), (1,)), ((), ())), preferred_element_type=jnp.float32
    )


def contract_first(left, right):
    return lax.dot_general(
        left, right, (((0,), (0,)), ((), ())), preferred_element_type=jnp.float32
    )


def slotted(tokens, out_grad, expert_ids, router_weight, w_gate, w_up, w_down):
    tok_dev, model_width = tokens.shape
    top_count = expert_ids.shape[1]
    expert_count = router_weight.shape[1]
    peer_count = lax.axis_size("ep")
    tp_count = lax.axis_size("tp")
    capacity = min(
        tok_dev,
        tp_count * max(1, (2 * tok_dev * top_count // expert_count + tp_count - 1) // tp_count),
    )
    feature_part = model_width // tp_count
    logits = jnp.dot(tokens, router_weight, preferred_element_type=jnp.float32)
    chosen = jnp.take_along_axis(logits, expert_ids, axis=1)
    gate_values = jax.nn.softmax(chosen, axis=-1)
    flat_ids = expert_ids.reshape(-1)
    one_hot = (flat_ids[:, None] == jnp.arange(expert_count, dtype=jnp.int32)[None, :]).astype(
        jnp.int32
    )
    slot_rank = jnp.sum((jnp.cumsum(one_hot, axis=0) - one_hot) * one_hot, axis=1)
    slot_index = flat_ids * capacity + slot_rank
    flat_tok = jnp.arange(tok_dev * top_count, dtype=jnp.int32) // top_count
    buffer_rows = expert_count * capacity
    sent_tokens = (
        jnp.zeros((buffer_rows, model_width), jnp.bfloat16).at[slot_index].set(tokens[flat_tok])
    )
    sent_grads = (
        jnp.zeros((buffer_rows, model_width), jnp.bfloat16).at[slot_index].set(out_grad[flat_tok])
    )
    sent_gates = jnp.zeros((buffer_rows,), jnp.float32).at[slot_index].set(gate_values.reshape(-1))
    slot_tokens = sent_tokens.reshape(expert_count, capacity, model_width)
    slot_grads = sent_grads.reshape(expert_count, capacity, model_width)
    slot_gates = sent_gates.reshape(expert_count, capacity)
    slot_share = capacity // tp_count
    share_start = lax.axis_index("tp") * slot_share
    part_tokens = lax.dynamic_slice_in_dim(slot_tokens, share_start, slot_share, 1)
    part_grads = lax.dynamic_slice_in_dim(slot_grads, share_start, slot_share, 1)
    part_gates = lax.dynamic_slice_in_dim(slot_gates, share_start, slot_share, 1)
    got_tokens, got_grads = (
        lax.all_to_all(part_tokens, "ep", split_axis=0, concat_axis=0, tiled=True),
        lax.all_to_all(part_grads, "ep", split_axis=0, concat_axis=0, tiled=True),
    )
    got_gates = lax.all_to_all(part_gates, "ep", split_axis=0, concat_axis=0, tiled=True)
    recv_tokens, recv_grads = (
        lax.all_gather(got_tokens, "tp", axis=1, tiled=True),
        lax.all_gather(got_grads, "tp", axis=1, tiled=True),
    )
    recv_gates = lax.all_gather(got_gates, "tp", axis=1, tiled=True)
    slot_count = peer_count * capacity
    inputs_rows = recv_tokens.reshape(slot_count, model_width)
    grad_rows = recv_grads.reshape(slot_count, model_width)
    weight_rows = recv_gates.reshape(slot_count)
    gate_mat = w_gate[0]
    up_mat = w_up[0]
    down_mat = w_down[0]
    gate_pre = jnp.dot(inputs_rows, gate_mat, preferred_element_type=jnp.float32)
    up_pre = jnp.dot(inputs_rows, up_mat, preferred_element_type=jnp.float32)
    hidden, slope, up_slope = activation_parts(gate_pre, up_pre)
    back_proj = contract_last(grad_rows, down_mat)
    gate_score = jnp.sum(hidden * back_proj, axis=1)
    d_hidden = weight_rows[:, None] * back_proj
    d_gate_pre = (d_hidden * slope).astype(jnp.bfloat16)
    d_up_pre = (d_hidden * up_slope).astype(jnp.bfloat16)
    weighted = (weight_rows[:, None] * hidden).astype(jnp.bfloat16)
    w_down_grad = contract_first(weighted, grad_rows).astype(jnp.bfloat16)[None]
    w_gate_grad = contract_first(inputs_rows, d_gate_pre).astype(jnp.bfloat16)[None]
    w_up_grad = contract_first(inputs_rows, d_up_pre).astype(jnp.bfloat16)[None]
    summed_part = lax.psum_scatter(
        contract_last(gate_mat, d_gate_pre) + contract_last(up_mat, d_up_pre),
        "tp",
        scatter_dimension=0,
        tiled=True,
    )
    returned = summed_part.T.reshape(peer_count, capacity, feature_part)
    home_grads, home_scores = (
        lax.all_to_all(returned, "ep", split_axis=0, concat_axis=0, tiled=True),
        lax.all_to_all(
            gate_score.reshape(peer_count, capacity), "ep", split_axis=0, concat_axis=0, tiled=True
        ),
    )
    picked = home_grads.reshape(buffer_rows, feature_part)[slot_index]
    expert_part = jnp.sum(picked.reshape(tok_dev, top_count, feature_part), axis=1)
    local_scores = home_scores.reshape(buffer_rows)[slot_index].reshape(tok_dev, top_count)
    total_scores = lax.psum(local_scores, "tp")
    d_chosen = gate_values * (
        total_scores - jnp.sum(gate_values * total_scores, axis=-1, keepdims=True)
    )
    expert_hot = (
        expert_ids[:, :, None] == jnp.arange(expert_count, dtype=jnp.int32)[None, None, :]
    ).astype(jnp.float32)
    d_logits = jnp.sum(d_chosen[:, :, None] * expert_hot, axis=1)
    column = lax.axis_index("tp") * feature_part
    local_tokens = lax.dynamic_slice_in_dim(tokens, column, feature_part, 1).astype(jnp.float32)
    router_term = jnp.dot(local_tokens.T, d_logits, precision=lax.Precision.HIGHEST)
    router_grad = lax.psum_scatter(router_term, "ep", scatter_dimension=1, tiled=True)
    router_rows = lax.dynamic_slice_in_dim(router_weight, column, feature_part, 0).astype(
        jnp.float32
    )
    router_part = jnp.dot(d_logits, router_rows.T, precision=lax.Precision.HIGHEST)
    token_grad = (expert_part + router_part).astype(jnp.bfloat16)
    return (token_grad, router_grad, w_gate_grad, w_up_grad, w_down_grad)


SCHEDULE = (
    ("z", 1), ("p", 0), ("z", 2), ("r",), ("m", 0), ("f", 0), ("p", 1), ("z", 3), ("q", 0),
    ("m", 1), ("f", 1), ("p", 2), ("am", 0), ("q", 1), ("m", 2), ("f", 2), ("p", 3), ("am", 1),
    ("q", 2), ("ap", 0), ("m", 3), ("f", 3), ("ts",), ("q", 3), ("am", 2), ("ap", 1), ("w", 2),
    ("am", 3), ("te",), ("w", 2), ("ap", 2), ("w", 4), ("ap", 3),
)


def dense_kernel(
    tok_ref, og_ref, ids_hbm, rw_hbm, wg_ref, wu_ref, wd_ref,
    tgrad_ref, rgrad_ref, wgg, wug, wdg,
    ids_ref, rw_ref, rows_v, wg, wu, wd, gates, dpre, weighted, part_scores, tp_scores, scores, dlog,
    own_part, mate_out, mate_in, p_out, p_in, z_out, z_in,
    load_sem, z_s, z_r, p_s, p_r, m_s, m_r,
    g_s, g_r, t_s, t_r, s_s, s_r, rm_s, rm_r, rp_s, rp_r, rz_s, rz_r,
):
    block, width = tok_ref.shape
    units = wd.shape[0]
    n_ep, experts, lanes = gates.shape
    n_tp = lax.axis_size("tp")
    n_z = n_ep // 2
    feat = width // n_tp
    ep = lax.axis_index("ep")
    tp = lax.axis_index("tp")
    z, y = ep // 2, ep % 2
    x, core = tp // 2, tp % 2
    y_dev = (z * 2 + 1 - y, tp)
    x_dev = (ep, (1 - x) * 2 + core)
    d_dev = (z * 2 + 1 - y, (1 - x) * 2 + core)
    m_dev = (ep, x * 2 + 1 - core)
    plane = (y_dev, x_dev, d_dev)
    near = (z, 1 + z % 2, (2 + 3 * z) % 5, 3 * (1 - z // 2))

    def z_dev(i):
        return (near[i] * 2 + y, tp)

    def ep_dev(hop):
        return ((ep + hop) % n_ep, tp)

    def tp_dev(hop):
        return (ep, (tp + hop) % n_tp)

    def remote(src, dst, send, recv, dev):
        return pltpu.make_async_remote_copy(
            src_ref=src, dst_ref=dst, send_sem=send, recv_sem=recv,
            device_id=dev, device_id_type=MESH,
        )

    def cols(quarter):
        return pl.ds(pl.multiple_of(quarter * feat, feat), feat)

    def rows(start, count):
        return pl.ds(pl.multiple_of(start * block, block), count * block)

    mine = rows(ep, 1)
    loads = [
        pltpu.make_async_copy(tok_ref, rows_v.at[0, mine, :], load_sem.at[0]),
        pltpu.make_async_copy(og_ref, rows_v.at[1, mine, :], load_sem.at[1]),
        pltpu.make_async_copy(ids_hbm, ids_ref, load_sem.at[2]),
        pltpu.make_async_copy(rw_hbm, rw_ref, load_sem.at[3]),
        pltpu.make_async_copy(wg_ref.at[0], wg, load_sem.at[4]),
        pltpu.make_async_copy(wu_ref.at[0], wu, load_sem.at[5]),
        pltpu.make_async_copy(wd_ref.at[0], wd, load_sem.at[6]),
    ]
    for load in loads:
        load.start()
    barrier = pltpu.get_barrier_semaphore()
    partners = [ep_dev(k) for k in range(1, n_ep)] + [tp_dev(k) for k in range(1, n_tp)] + [d_dev]
    for dev in partners:
        pl.semaphore_signal(barrier, inc=1, device_id=dev, device_id_type=MESH)
    pl.semaphore_wait(barrier, len(partners))
    sent = []

    def launch(copy):
        copy.start()
        sent.append(copy)

    own_q, other_q = cols(tp), cols((1 - x) * 2 + core)
    mate_q = (cols(x * 2 + 1 - core), cols((1 - x) * 2 + 1 - core))

    def piece(first, count, quarter):
        return rows_v.at[:, rows(first, count), quarter]

    def z_send(i):
        p = piece(ep, 1, own_q)
        return remote(p, p, z_s.at[i], z_r.at[z], z_dev(i))

    def z_recv(i):
        p = piece(near[i] * 2 + y, 1, own_q)
        return remote(p, p, z_s.at[i], z_r.at[near[i]], z_dev(i))

    def p_copy(i, kind, first, quarter=None):
        p = piece(first, 1, own_q if quarter is None else quarter)
        return remote(p, p, p_s.at[i, kind], p_r.at[i, kind], plane[min(kind, 2)])

    def m_copy(i, which, first, count, quarter):
        p = piece(first, count, quarter)
        return remote(p, p, m_s.at[i, which], m_r.at[i, which], m_dev)

    def y_home(which, first, quarter):
        p = piece(first, 1, quarter)
        return remote(p, p, p_s.at[0, which], p_r.at[0, which], y_dev)

    loads[0].wait()
    loads[1].wait()
    launch(y_home(0, ep, own_q))
    for i in range(1, n_z):
        launch(z_send(i))
    launch(y_home(1, ep, other_q))

    loads[2].wait()
    loads[3].wait()
    logits = contract_last(rw_ref[...], rows_v[0, mine, :])
    expert = lax.broadcasted_iota(jnp.int32, (experts, block), 0)
    hot = jnp.zeros((experts, block), jnp.float32)
    for k in range(ids_ref.shape[0]):
        hot = jnp.where(ids_ref[k : k + 1, :] == expert, 1.0, hot)
    top = jnp.max(jnp.where(hot > 0.0, logits, -jnp.inf), axis=0, keepdims=True)
    expd = jnp.where(hot > 0.0, jnp.exp(jnp.where(hot > 0.0, logits - top, 0.0)), 0.0)
    gate_rows = expd / jnp.sum(expd, axis=0, keepdims=True)
    gates[ep] = jnp.zeros((experts, lanes), jnp.float32)
    gates[ep, :, 0:block] = gate_rows

    def gate_copy(hop, src):
        return remote(gates.at[src], gates.at[src], g_s.at[hop], g_r.at[hop], ep_dev(hop))

    for hop in range(1, n_ep):
        launch(gate_copy(hop, ep))

    def pair(i):
        return near[i] * 2 + y, near[i] * 2 + 1 - y

    def z_event(i):
        a, _ = pair(i)
        z_recv(i).wait_recv()
        for kind in range(3):
            launch(p_copy(i, kind, a))
        launch(m_copy(i, 0, a, 1, own_q))

    def plane_event(i):
        a, b = pair(i)
        if i == 0:
            y_home(0, b, own_q).wait_recv()
            launch(m_copy(0, 1, b, 1, own_q))
            y_home(1, b, other_q).wait_recv()
            launch(m_copy(0, 2, b, 1, other_q))
        else:
            p_copy(i, 0, b).wait_recv()
            launch(m_copy(i, 1, b, 1, own_q))
            p_copy(i, 1, a, other_q).wait_recv()
            p_copy(i, 2, b, other_q).wait_recv()
            launch(m_copy(i, 2, near[i] * 2, 2, other_q))

    def mate_event(i):
        a, b = pair(i)
        m_copy(i, 1, b, 1, mate_q[0]).wait_recv()
        if i == 0:
            m_copy(i, 2, b, 1, mate_q[1]).wait_recv()
        else:
            m_copy(i, 0, a, 1, mate_q[0]).wait_recv()
            m_copy(i, 2, near[i] * 2, 2, mate_q[1]).wait_recv()

    def forward(i):
        zs = near[i]
        here = rows(zs * 2, 2)
        in_rows = rows_v[0, here, :]
        grad_rows = rows_v[1, here, :]
        gate_pre = jnp.dot(in_rows, wg[...], preferred_element_type=jnp.float32)
        up_pre = jnp.dot(in_rows, wu[...], preferred_element_type=jnp.float32)
        back = contract_last(grad_rows, wd[...])
        hidden, slope, up_slope = activation_parts(gate_pre, up_pre)
        columns = []
        for k in range(2):
            row = gates[zs * 2 + k, pl.ds(ep, 1), :]
            columns.append(jnp.broadcast_to(row, (lanes, lanes)).T[:block])
        weight = jnp.concatenate(columns, axis=0)
        weight = jnp.concatenate([weight] * (units // lanes), axis=1)
        product = hidden * back
        folded = product[:, 0:lanes]
        for k in range(1, units // lanes):
            folded = folded + product[:, k * lanes : (k + 1) * lanes]
        for k in range(2):
            tall = jnp.concatenate(
                [folded[k * block : (k + 1) * block], jnp.zeros((lanes - block, lanes), jnp.float32)],
                axis=0,
            )
            part_scores[pl.ds(zs * 2 + k, 1), :] = jnp.sum(tall.T, axis=0, keepdims=True)
        d_hidden = weight * back
        dpre[here, 0:units] = (d_hidden * slope).astype(jnp.bfloat16)
        dpre[here, units : 2 * units] = (d_hidden * up_slope).astype(jnp.bfloat16)
        weighted[here, :] = (weight * hidden).astype(jnp.bfloat16)

    def tp_score_copy(hop):
        return remote(part_scores, tp_scores.at[hop], t_s.at[hop], t_r.at[hop], tp_dev(hop))

    def score_copy(hop, src):
        return remote(scores.at[src], scores.at[src], s_s.at[hop], s_r.at[hop], ep_dev(hop))

    def back_mate(i):
        return remote(mate_out.at[i], mate_in.at[i], rm_s.at[i], rm_r.at[i], m_dev)

    def back_plane(i, kind):
        return remote(p_out.at[i, kind], p_in.at[i, kind], rp_s.at[i, kind], rp_r.at[i, kind], plane[kind])

    def back_send(i):
        return remote(z_out.at[i], z_in.at[z], rz_s.at[i], rz_r.at[z], z_dev(i))

    def back_recv(i):
        return remote(z_out.at[i], z_in.at[near[i]], rz_s.at[i], rz_r.at[near[i]], z_dev(i))

    def produce(i):
        here = rows(near[i] * 2, 2)
        dg = dpre[here, 0:units]
        du = dpre[here, units : 2 * units]
        for side in range(2):
            for half in range(2):
                q = half * 2 + (1 - core if side == 0 else core)
                span = cols(q)
                value = contract_last(dg, wg[span, :]) + contract_last(du, wu[span, :])
                if side == 0:
                    mate_out[i, half] = value.astype(jnp.bfloat16)
                else:
                    own_part[i, half] = value
            if side == 0:
                launch(back_mate(i))

    def after_mate(i):
        back_mate(i).wait_recv()
        ours, theirs = rows(y, 1), rows(1 - y, 1)
        for kind, (half, part) in enumerate(((x, theirs), (1 - x, ours), (1 - x, theirs))):
            p_out[i, kind] = (
                own_part[i, half, part, :] + mate_in[i, half, part, :].astype(jnp.float32)
            ).astype(jnp.bfloat16)
            launch(back_plane(i, kind))

    home = {}

    def after_plane(i):
        ours = rows(y, 1)
        total = own_part[i, x, ours, :] + mate_in[i, x, ours, :].astype(jnp.float32)
        for kind in range(3):
            back_plane(i, kind).wait_recv()
            total = total + p_in[i, kind].astype(jnp.float32)
        if i > 0:
            z_out[i] = total.astype(jnp.bfloat16)
            launch(back_send(i))
        else:
            own_part[0, x, ours, :] = total

    tiles = 8
    tile = width // tiles

    def in_grad(i):
        span = pl.ds(i * tile, tile)
        value = contract_first(rows_v[0, :, span], dpre[...]).astype(jnp.bfloat16)
        wgg[0, span, :] = value[:, 0:units]
        wug[0, span, :] = value[:, units : 2 * units]

    def down_grad(i):
        span = pl.ds(i * feat, feat)
        wdg[0, :, span] = contract_first(weighted[...], rows_v[1, :, span]).astype(jnp.bfloat16)

    pieces = [functools.partial(in_grad, i) for i in range(tiles)]
    pieces += [functools.partial(down_grad, i) for i in range(n_tp)]

    def work(amount):
        for piece in pieces[:amount]:
            piece()
        del pieces[:amount]

    def ready():
        for hop in range(1, n_ep):
            gate_copy(hop, (ep + n_ep - hop) % n_ep).wait_recv()
        for load in loads[4:]:
            load.wait()

    def tp_send():
        for hop in range(1, n_tp):
            launch(tp_score_copy(hop))

    def tp_event():
        total = part_scores[...]
        for hop in range(1, n_tp):
            tp_score_copy(hop).wait_recv()
            total = total + tp_scores[hop]
        scores[ep] = total
        for hop in range(1, n_ep):
            launch(score_copy(hop, ep))

    steps = {
        "z": z_event, "p": plane_event, "m": mate_event, "f": forward, "q": produce,
        "am": after_mate, "ap": after_plane, "w": work,
    }
    for name, *args in SCHEDULE:
        {**steps, "r": ready, "ts": tp_send, "te": tp_event}[name](*args)
    work(len(pieces))
    for hop in range(1, n_ep):
        score_copy(hop, (ep + n_ep - hop) % n_ep).wait_recv()
    score = scores[...]
    my_row = lax.broadcasted_iota(jnp.int32, (experts, lanes), 0) == ep
    router = jnp.zeros((experts, feat), jnp.float32)
    for s in range(n_ep):
        gate = gates[s]
        here = score[:, s, :]
        d_log = gate * (here - jnp.sum(gate * here, axis=0, keepdims=True))
        dlog[s] = d_log
        router = router + jnp.dot(
            jnp.where(my_row, d_log, 0.0)[:, 0:block],
            rows_v[0, s * block : (s + 1) * block, own_q].astype(jnp.float32),
            precision=lax.Precision.HIGHEST,
            preferred_element_type=jnp.float32,
        )
    rgrad_ref[...] = jnp.sum(router, axis=0, keepdims=True)
    term = jnp.dot(
        dlog[ep].T[0:block],
        rw_ref[:, own_q].astype(jnp.float32),
        precision=lax.Precision.HIGHEST,
        preferred_element_type=jnp.float32,
    )
    result = own_part[0, x, rows(y, 1), :] + term
    for i in range(1, n_z):
        back_recv(i).wait_recv()
        result = result + z_in[near[i]].astype(jnp.float32)
    tgrad_ref[...] = result.astype(jnp.bfloat16)
    for copy in sent:
        copy.wait_send()


def write_out(*refs):
    count = len(refs) // 2
    copies = [
        pltpu.make_async_copy(refs[i], refs[count + i], refs[-1].at[i]) for i in range(count)
    ]
    for copy in reversed(copies):
        copy.start()
    for copy in copies:
        copy.wait()


def dense(tokens, out_grad, expert_ids, router_weight, w_gate, w_up, w_down):
    block, width = tokens.shape
    units = w_gate.shape[2]
    top_count = expert_ids.shape[1]
    experts = router_weight.shape[1]
    n_ep, n_tp = lax.axis_size("ep"), lax.axis_size("tp")
    n_z = n_ep // 2
    feat = width // n_tp
    count = n_ep * block
    lanes = 128
    bf16, f32 = jnp.bfloat16, jnp.float32
    vmem = pl.BlockSpec(memory_space=pltpu.VMEM)
    hbm = pl.BlockSpec(memory_space=pltpu.HBM)
    dma = pltpu.SemaphoreType.DMA
    results = (
        ((block, feat), bf16),
        ((1, feat), f32),
        (w_gate.shape, bf16),
        (w_up.shape, bf16),
        (w_down.shape, bf16),
    )
    held = pl.pallas_call(
        dense_kernel,
        out_shape=tuple(pltpu.VMEM(shape, kind) for shape, kind in results),
        in_specs=[hbm] * 7,
        out_specs=(vmem,) * len(results),
        scratch_shapes=[
            pltpu.VMEM((top_count, block), jnp.int32),
            pltpu.VMEM((experts, width), bf16),
            pltpu.VMEM((2, count, width), bf16),
            pltpu.VMEM((width, units), bf16),
            pltpu.VMEM((width, units), bf16),
            pltpu.VMEM((units, width), bf16),
            pltpu.VMEM((n_ep, experts, lanes), f32),
            pltpu.VMEM((count, 2 * units), bf16),
            pltpu.VMEM((count, units), bf16),
            pltpu.VMEM((n_ep, lanes), f32),
            pltpu.VMEM((n_tp, n_ep, lanes), f32),
            pltpu.VMEM((experts, n_ep, lanes), f32),
            pltpu.VMEM((n_ep, experts, lanes), f32),
            pltpu.VMEM((n_z, 2, 2 * block, feat), f32),
            pltpu.VMEM((n_z, 2, 2 * block, feat), bf16),
            pltpu.VMEM((n_z, 2, 2 * block, feat), bf16),
            pltpu.VMEM((n_z, 3, block, feat), bf16),
            pltpu.VMEM((n_z, 3, block, feat), bf16),
            pltpu.VMEM((n_z, block, feat), bf16),
            pltpu.VMEM((n_z, block, feat), bf16),
            dma((7,)),
            dma((n_z,)), dma((n_z,)), dma((n_z, 3)), dma((n_z, 3)), dma((n_z, 3)), dma((n_z, 3)),
            dma((n_ep,)), dma((n_ep,)), dma((n_tp,)), dma((n_tp,)), dma((n_ep,)), dma((n_ep,)),
            dma((n_z,)), dma((n_z,)), dma((n_z, 3)), dma((n_z, 3)), dma((n_z,)), dma((n_z,)),
        ],
        compiler_params=pltpu.CompilerParams(
            collective_id=0, has_side_effects=True, vmem_limit_bytes=40 * 1024 * 1024
        ),
    )(
        *[
            pltpu.with_memory_space_constraint(part, pltpu.HBM)
            for part in (tokens, out_grad, expert_ids.T, router_weight.T, w_gate, w_up, w_down)
        ],
    )
    outs = pl.pallas_call(
        write_out,
        out_shape=tuple(jax.ShapeDtypeStruct(shape, kind) for shape, kind in results),
        in_specs=[vmem] * len(results),
        out_specs=(hbm,) * len(results),
        scratch_shapes=[dma((len(results),))],
        compiler_params=pltpu.CompilerParams(vmem_limit_bytes=16 * 1024 * 1024),
    )(*[pltpu.with_memory_space_constraint(part, pltpu.VMEM) for part in held])
    token_grad, router_grad, w_gate_grad, w_up_grad, w_down_grad = outs
    return (token_grad, router_grad.T, w_gate_grad, w_up_grad, w_down_grad)


def per_device(tokens, out_grad, expert_ids, router_weight, w_gate, w_up, w_down):
    tok_dev, top_count = expert_ids.shape
    expert_count = router_weight.shape[1]
    tp_count = lax.axis_size("tp")
    capacity = min(
        tok_dev,
        tp_count * max(1, (2 * tok_dev * top_count // expert_count + tp_count - 1) // tp_count),
    )
    full = capacity == tok_dev and tp_count == 4 and lax.axis_size("ep") == 8
    return (dense if full else slotted)(
        tokens, out_grad, expert_ids, router_weight, w_gate, w_up, w_down
    )


def solution(mesh):
    in_specs = (
        P("ep", None),
        P("ep", None),
        P("ep", None),
        P(),
        P("ep", None, "tp"),
        P("ep", None, "tp"),
        P("ep", "tp", None),
    )
    out_specs = (
        P("ep", "tp"),
        P("tp", "ep"),
        P("ep", None, "tp"),
        P("ep", None, "tp"),
        P("ep", "tp", None),
    )
    return jax.shard_map(
        per_device, mesh=mesh, in_specs=in_specs, out_specs=out_specs, check_vma=False
    )
```
